32 devices in a mesh: ep: 8 (over z, core), tp: 4 (over y, x).
Axes of the slice: x: 2, y: 2, z: 4, core: 2. Of those that a mesh axis runs over, the one named last changes fastest.
Arguments:
- tokens: bfloat16 [2048, 2048], P('ep'), may hold values from -6 to 6
- norm_gain: float32 [2048], replicated, may hold values from 0.1 to 1.9
- route_ids: int32 [2048, 4], P('ep'), may hold values from 0 to 15, all different within a row; in each aligned block of 256 rows (0 to 255, 256 to 511, ...) at most 96 rows name the same one
- route_weights: float32 [2048, 4], P('ep'), may hold values from 0.1 to 1
- w_gate: bfloat16 [16, 2048, 2048], P('ep', None, 'tp'), may hold values from -0.33007812 to 0.33007812
- w_up: bfloat16 [16, 2048, 2048], P('ep', None, 'tp'), may hold values from -0.33007812 to 0.33007812
- w_down: bfloat16 [16, 2048, 2048], P('ep', None, 'tp'), may hold values from -0.026489258 to 0.026489258
Outputs:
- mixed_out: bfloat16 [2048, 2048], P('ep', 'tp')
The draws below stay inside these ranges and needn't reach their ends.
Inputs may be any that keep to these rules, and one draw needn't show every extreme that they name: `route_ids`: each token names 4 different experts. Within the tokens of one index of ep (aligned blocks of 256 tokens) no expert is named more than 96 times, a bound that some block reaches.
All inputs are finite; a program needn't handle non-finite values.
Results may differ from the reference program's by a relative error of at most 0.007.
Values may be sent and summed in bfloat16 or wider, within the bound.
A program may use at most 64 MiB of HBM per device.

```python
import math
import jax
import jax.numpy as jnp
import numpy as np
from jax import lax

D = 2048
FF = 2048
TOP_K = 4
TOK_DEV = 256
EXPERTS = 16
TOKENS = 2048
CAP = 96
N_EP = 8


def block_scale(rng, shape, split, smallest, top_value):
    def one(axis_at, parts):
        heights = jax.random.uniform(jax.random.fold_in(jax.random.fold_in(rng, 6), axis_at), (parts,), jnp.float32, smallest / len(split), top_value / len(split))
        return jnp.repeat(jnp.exp(heights), shape[axis_at] // parts).reshape((-1,) + (1,) * (len(shape) - axis_at - 1))

    level = one(*split[0])
    for cut in split[1:]:
        level = level * one(*cut)
    return level


def assign_block(own_key, own, number, rows, amount, top, reach, lean):
    ranking = jax.random.permutation(own_key, amount)
    crowded, ordinary = load_shares(amount, rows * top, reach, lean, True), load_shares(amount, rows * top, reach, lean, False)
    places = jnp.arange(amount)

    def named(tallies, offset_by):
        used = int((tallies > 0).sum())
        fixed = max(1, used // 4)
        passed = fixed + (places - fixed + offset_by * (used - fixed)) % max(1, amount - fixed)
        return jnp.zeros((amount,), jnp.int32).at[ranking[jnp.where(places < fixed, places, passed)]].set(jnp.asarray(tallies, jnp.int32))

    tallies = jnp.where(number % 4 == 0, named(crowded, number // 4), named(ordinary, number - number // 4 - 1))
    mixed = jax.random.permutation(jax.random.fold_in(own, 3), amount)
    giver, sink = mixed[0:amount // 2 * 2:2], mixed[1:amount // 2 * 2:2]
    room = jnp.minimum(tallies[giver] - 1, reach - tallies[sink]) // 2
    room = jnp.where((giver == ranking[0]) | (sink == ranking[0]) | (tallies[sink] == 0), 0, jnp.maximum(room, 0))
    passed = jax.random.randint(jax.random.fold_in(own, 4), (amount // 2,), 0, 1 << 20) % (room + 1)
    tallies = tallies.at[giver].add(-passed).at[sink].add(passed)
    members = jnp.searchsorted(jnp.cumsum(tallies), jnp.arange(rows * top), side="right").astype(jnp.int32)
    listing = members.reshape(top, rows).T
    listing = listing[jax.random.permutation(jax.random.fold_in(own, 1), rows)]
    offset_by = jax.random.randint(jax.random.fold_in(own, 2), (rows, 1), 0, top)
    return jnp.take_along_axis(listing, (jnp.arange(top)[None, :] + offset_by) % top, axis=1)


def load_shares(number_of, total, reach, slope, full):
    portions = [(1 << 20) // math.isqrt(grade ** slope) + 1 for grade in range(1, number_of + 1)]
    largest = reach if full else min(reach, max(-(-total // number_of), total * portions[0] // sum(portions)))
    least = 1 if total - largest >= number_of - 1 else 0
    counts, spare = [largest] + [least] * (number_of - 1), total - largest - least * (number_of - 1)
    while spare > 0:
        free = [i for i in range(1, number_of) if counts[i] < largest] or [i for i in range(1, number_of) if counts[i] < reach]
        whole, remaining = sum([portions[i] for i in free]), spare
        for i in free:
            extra = min(reach - counts[i], max(1, remaining * portions[i] // whole), spare)
            counts[i] = counts[i] + extra
            spare = spare - extra
    return np.array(counts)


def scatter_about(own_key, extent, scale, limit, split=(), kind=jnp.bfloat16):
    entries = scale * jax.random.normal(own_key, extent, jnp.float32)
    if split:
        entries = entries * block_scale(own_key, extent, split, -0.22, 0.18)
    return jnp.clip(entries, -limit, limit).astype(kind)


def setup_inputs(seed: int = 0) -> dict:
    splits = jax.random.split(jax.random.key(seed), 8)
    tokens = scatter_about(splits[0], (TOKENS, D), 1.0, 6.0, ((0, 8),))
    norm_gain = jnp.clip(1.0 + 0.18 * jax.random.normal(splits[1], (D,), jnp.float32), 0.1, 1.9)
    route_ids_keys = jax.random.split(jax.random.fold_in(splits[2], 1), TOKENS // TOK_DEV)
    route_ids_turns = jax.random.permutation(jax.random.fold_in(splits[2], 3), TOKENS // TOK_DEV)
    route_ids = jax.vmap(lambda own, number: assign_block(jax.random.fold_in(splits[2], 2), own, number, TOK_DEV, EXPERTS, TOP_K, CAP, 2))(route_ids_keys, route_ids_turns).reshape((TOKENS, TOP_K))
    route_weights = jnp.clip(0.1 + 0.9 * jax.random.uniform(splits[3], (TOKENS, TOP_K), jnp.float32) ** block_scale(splits[3], (TOKENS, TOP_K), ((0, 8),), -0.2, 0.2), 0.1, 1.0)
    w_gate = scatter_about(splits[4], (EXPERTS, D, FF), (2.5 * D ** -0.5), 0.33007812, ((0, 8), (2, 4)))
    w_up = scatter_about(splits[5], (EXPERTS, D, FF), (2.5 * D ** -0.5), 0.33007812, ((0, 8), (2, 4)))
    w_down = scatter_about(splits[6], (EXPERTS, FF, D), (0.2 * FF ** -0.5), 0.026489258, ((0, 8), (2, 4)))
    return {"tokens": tokens, "norm_gain": norm_gain, "route_ids": route_ids, "route_weights": route_weights, "w_gate": w_gate, "w_up": w_up, "w_down": w_down}


swiglu_limit = 7.0
swiglu_alpha = 1.702
norm_eps = 1e-05

def clamped_units(gate_pre, up_pre):
    capped = jnp.minimum(gate_pre, swiglu_limit)
    linear = jnp.clip(up_pre, -swiglu_limit, swiglu_limit)
    return capped * jax.nn.sigmoid(swiglu_alpha * capped) * (linear + 1.0)

def slots_of(group_ids):
    matches = (group_ids[:, None] == jnp.arange(EXPERTS, dtype=jnp.int32)[None, :]).astype(jnp.int32)
    earlier = jnp.cumsum(matches, axis=0) - matches
    return lax.optimization_barrier(jnp.sum(earlier * matches, axis=1)).astype(jnp.int32)

def one_expert(args):
    row_block, gate_weight, up_weight, down_weight = args
    row_values = row_block.astype(jnp.float32)
    gate_pre = jnp.dot(row_values, gate_weight.astype(jnp.float32), preferred_element_type=jnp.float32)
    up_pre = jnp.dot(row_values, up_weight.astype(jnp.float32), preferred_element_type=jnp.float32)
    activation = clamped_units(gate_pre, up_pre).astype(jnp.bfloat16)
    result = jnp.dot(activation.astype(jnp.float32), down_weight.astype(jnp.float32), preferred_element_type=jnp.float32)
    return result.astype(jnp.bfloat16)

def reference(tokens, norm_gain, route_ids, route_weights, w_gate, w_up, w_down):
    values = tokens.astype(jnp.float32)
    row_mean = lax.optimization_barrier(jnp.mean(values, axis=1, keepdims=True))
    centred = values - row_mean
    row_var = lax.optimization_barrier(jnp.mean(centred * centred, axis=1, keepdims=True))
    normed = (centred * lax.rsqrt(row_var + norm_eps) * norm_gain).astype(jnp.bfloat16)
    group_ids = route_ids.reshape(N_EP, TOK_DEV * TOP_K).astype(jnp.int32)
    slot_index = lax.map(slots_of, group_ids)
    group_rank = jnp.arange(N_EP, dtype=jnp.int32)[:, None]
    position = (group_ids * (N_EP * CAP) + group_rank * CAP + slot_index).reshape(-1).astype(jnp.int32)
    source_rows = jnp.repeat(normed, TOP_K, axis=0)
    buffer = jnp.zeros((EXPERTS * N_EP * CAP, D), jnp.bfloat16).at[position].set(source_rows)
    results = lax.map(one_expert, (buffer.reshape(EXPERTS, N_EP * CAP, D), w_gate, w_up, w_down))
    picked = results.reshape(EXPERTS * N_EP * CAP, D)[position].reshape(TOKENS, TOP_K, D).astype(jnp.float32)
    return lax.optimization_barrier(jnp.sum(picked * route_weights[:, :, None], axis=1)).astype(jnp.bfloat16)
```

```python
import functools
import jax
import jax.numpy as jnp
from jax import lax
from jax.experimental import pallas as pl
from jax.experimental.pallas import tpu as pltpu
from jax.sharding import PartitionSpec as P

swiglu_limit = 7.0
swiglu_alpha = 1.702
norm_eps = 1e-05


def clamped_units(gate_pre, up_pre):
    capped = jnp.minimum(gate_pre, swiglu_limit)
    linear = jnp.clip(up_pre, -swiglu_limit, swiglu_limit)
    return capped * jax.nn.sigmoid(swiglu_alpha * capped) * (linear + 1.0)


def expert_work(outgoing, gate_weight, up_weight, down_weight):
    received = lax.all_to_all(outgoing, "ep", split_axis=1, concat_axis=1, tiled=True)
    local_count, sources, capacity, columns = received.shape
    row_count = sources * capacity
    row_block = received.reshape(local_count, row_count, columns)
    shard_piece = lax.all_gather(row_block, "tp", axis=2, tiled=True)
    gate_sum = jnp.einsum(
        "lrd,ldf->lrf", shard_piece, gate_weight, preferred_element_type=jnp.float32
    )
    up_sum = jnp.einsum("lrd,ldf->lrf", shard_piece, up_weight, preferred_element_type=jnp.float32)
    activation = clamped_units(gate_sum, up_sum).astype(jnp.bfloat16)
    out_cols = down_weight.shape[2]
    result = jnp.einsum(
        "lrf,lfd->lrd",
        lax.all_gather(activation, "tp", axis=2, tiled=True),
        down_weight,
        preferred_element_type=jnp.float32,
    )
    result = result.astype(jnp.bfloat16).reshape(local_count, sources, capacity, out_cols)
    return lax.all_to_all(result, "ep", split_axis=1, concat_axis=1, tiled=True)


def per_device(tokens, norm_gain, route_ids, route_weights, w_gate, w_up, w_down):
    local_count = w_gate.shape[0]
    sources = lax.axis_size("ep")
    tp_count = lax.axis_size("tp")
    width = tokens.shape[1]
    columns = width // tp_count
    experts = local_count * sources
    tok_rows, top_count = route_ids.shape
    capacity = 3 * tok_rows * top_count // (2 * experts)
    values = tokens.astype(jnp.float32)
    row_mean = jnp.mean(values, axis=1, keepdims=True)
    centred = values - row_mean
    row_var = jnp.mean(centred * centred, axis=1, keepdims=True)
    offset = lax.axis_index("tp") * columns
    own_cols = lax.dynamic_slice_in_dim(centred, offset, columns, 1)
    own_gain = lax.dynamic_slice_in_dim(norm_gain, offset, columns, 0)
    normed = (own_cols * lax.rsqrt(row_var + norm_eps) * own_gain).astype(jnp.bfloat16)
    flat_ids = route_ids.reshape(-1)
    matches = (flat_ids[:, None] == jnp.arange(experts, dtype=jnp.int32)[None, :]).astype(jnp.int32)
    earlier = jnp.cumsum(matches, axis=0) - matches
    slot_index = jnp.sum(earlier * matches, axis=1)
    position = (
        flat_ids % local_count * (sources * capacity)
        + flat_ids // local_count * capacity
        + slot_index
    )
    buffer_rows = local_count * sources * capacity
    placed = (
        position.reshape(tok_rows, top_count)[:, :, None]
        == jnp.arange(buffer_rows, dtype=jnp.int32)[None, None, :]
    )
    placement_matrix = jnp.any(placed, axis=1).astype(jnp.bfloat16)
    outgoing = jnp.einsum("tp,td->pd", placement_matrix, normed, preferred_element_type=jnp.float32)
    outgoing = outgoing.astype(jnp.bfloat16).reshape(local_count, sources, capacity, columns)
    returned = jnp.concatenate(
        [
            expert_work(
                outgoing[number : number + 1],
                w_gate[number : number + 1],
                w_up[number : number + 1],
                w_down[number : number + 1],
            )
            for number in range(local_count)
        ],
        axis=0,
    )
    flat_out = returned.reshape(buffer_rows, columns)
    picked = flat_out[position].reshape(tok_rows, top_count, columns).astype(jnp.float32)
    return jnp.sum(picked * route_weights[:, :, None], axis=1).astype(jnp.bfloat16)


def layer_kernel(
    capacity,
    normed_ref,
    meta_ref,
    gate_hbm,
    up_hbm,
    down_hbm,
    out_ref,
    gate_w,
    up_w,
    down_w,
    toks,
    meta_in,
    rows,
    acts,
    weighted,
    pair_out,
    pair_in,
    back_out,
    back_in,
    total_ref,
    weight_sem,
    local_sem,
    meta_send,
    meta_recv,
    line_send,
    line_recv,
    side_send,
    side_recv,
    pair_send,
    pair_recv,
    act_send,
    act_recv,
    sum_send,
    sum_recv,
    back_send,
    back_recv,
):
    sources = meta_ref.shape[0]
    chips = sources // 2
    local_count = gate_w.shape[0]
    units = gate_w.shape[2]
    tok_rows = normed_ref.shape[1]
    me = lax.axis_index("ep")
    tp = lax.axis_index("tp")
    z, core = me // 2, me % 2
    y, x = tp // 2, tp % 2
    tp_x = y * 2 + (1 - x)
    tp_y = (1 - y) * 2 + x
    tp_xy = (1 - y) * 2 + (1 - x)
    mate = z * 2 + (1 - core)

    def partner(k):
        other, bit, left = 0 * z, 1, z
        while bit < chips:
            digit = left % 2
            other = other + bit * ((1 - digit) if k & bit else digit)
            left, bit = left // 2, bit * 2
        return other

    def place(ep, column):
        return {"ep": ep, "tp": column}

    def remote(source, target, send, recv, where):
        return pltpu.make_async_remote_copy(
            src_ref=source,
            dst_ref=target,
            send_sem=send,
            recv_sem=recv,
            device_id=where,
            device_id_type=pl.DeviceIdType.MESH,
        )

    loads = []
    for n, (hbm, vmem) in enumerate(((gate_hbm, gate_w), (up_hbm, up_w), (down_hbm, down_w))):
        loads.append(pltpu.make_async_copy(hbm, vmem, weight_sem.at[n]))
        loads[-1].start()
    own_tok = pltpu.make_async_copy(normed_ref, toks.at[me], local_sem.at[0])
    own_tok.start()
    own_meta = pltpu.make_async_copy(meta_ref.at[me], meta_in.at[me], local_sem.at[1])
    own_meta.start()

    barrier = pltpu.get_barrier_semaphore()
    for d in range(1, sources):
        pl.semaphore_signal(
            barrier, inc=1, device_id=place((me + d) % sources, tp), device_id_type=pl.DeviceIdType.MESH
        )
    for column in (tp_x, tp_y):
        pl.semaphore_signal(
            barrier, inc=1, device_id=place(me, column), device_id_type=pl.DeviceIdType.MESH
        )
    pl.semaphore_wait(barrier, sources + 1)

    pending = []

    def go(copy):
        copy.start()
        pending.append(copy)
        return copy

    metas = [
        go(
            remote(
                meta_ref.at[(me + d) % sources],
                meta_in.at[me],
                meta_send.at[d],
                meta_recv.at[d],
                place((me + d) % sources, tp),
            )
        )
        for d in range(1, sources)
    ]
    own_pair = go(
        remote(normed_ref, toks.at[me], pair_send.at[0], pair_recv.at[0], place(mate, tp))
    )
    lines = {
        k: go(
            remote(
                normed_ref.at[x],
                toks.at[me, x],
                line_send.at[k],
                line_recv.at[k],
                place(partner(k) * 2 + core, tp),
            )
        )
        for k in range(1, chips)
    }

    pairs, sides, half_pairs = {}, {}, {}

    def spread_line(k):
        src = partner(k) * 2 + core
        lines[k].wait_recv()
        piece = toks.at[src, x]
        sides[k] = go(remote(piece, piece, side_send.at[k], side_recv.at[k], place(me, tp_x)))
        pairs[k] = go(
            remote(piece, piece, pair_send.at[2 * k], pair_recv.at[2 * k], place(mate, tp))
        )

    def spread_side(k):
        src = partner(k) * 2 + core
        sides[k].wait_recv()
        piece = toks.at[src, 1 - x]
        half_pairs[k] = go(
            remote(piece, piece, pair_send.at[2 * k + 1], pair_recv.at[2 * k + 1], place(mate, tp))
        )
        pairs[k].wait_recv()
        half_pairs[k].wait_recv()

    def chosen(source):
        slots = meta_in[source]
        at = lax.broadcasted_iota(jnp.int32, (capacity, tok_rows), 0).astype(jnp.float32)
        hits = [at == slots[n : n + 1, :] for n in range(local_count)]
        ones = jnp.concatenate([h.astype(jnp.float32) for h in hits], axis=0)
        scale = jnp.concatenate(
            [
                jnp.sum(
                    jnp.where(hits[n], slots[local_count + n : local_count + n + 1, :], 0.0),
                    axis=1,
                    keepdims=True,
                )
                for n in range(local_count)
            ],
            axis=0,
        )
        return ones.astype(jnp.bfloat16), scale

    halves = toks.shape[1]
    width = toks.shape[3]

    def first_half(k):
        s = partner(k)

        @pl.loop(0, 2)
        def _(j):
            ones, _ = chosen(2 * s + j)
            for h in range(halves):
                got = jnp.dot(ones, toks[2 * s + j, h], preferred_element_type=jnp.float32)
                got = got.astype(jnp.bfloat16)
                for n in range(local_count):
                    rows[n, j, :, h * width : (h + 1) * width] = got[
                        n * capacity : (n + 1) * capacity
                    ]

        @pl.loop(0, local_count)
        def _(n):
            block = rows[n].reshape(2 * capacity, halves * width)
            cut = units // 2
            for part in range(2):
                cols = slice(part * cut, (part + 1) * cut)
                gate = jnp.dot(block, gate_w[n, :, cols], preferred_element_type=jnp.float32)
                up = jnp.dot(block, up_w[n, :, cols], preferred_element_type=jnp.float32)
                acts[k, tp, n, :, cols] = clamped_units(gate, up).astype(jnp.bfloat16)

    own_x, own_y, fwd_y = {}, {}, {}

    def send_act(k):
        piece = acts.at[k, tp]
        own_x[k] = go(
            remote(piece, piece, act_send.at[k, 0], act_recv.at[k, 0], place(me, tp_x))
        )
        own_y[k] = go(
            remote(piece, piece, act_send.at[k, 1], act_recv.at[k, 1], place(me, tp_y))
        )

    def forward_act(k):
        own_x[k].wait_recv()
        piece = acts.at[k, tp_x]
        fwd_y[k] = go(
            remote(piece, piece, act_send.at[k, 2], act_recv.at[k, 2], place(me, tp_y))
        )

    sums = {}

    def second_half(k):
        s = partner(k)
        own_y[k].wait_recv()
        fwd_y[k].wait_recv()

        @pl.loop(0, local_count)
        def _(n):
            total = jnp.zeros((2 * capacity, down_w.shape[2]), jnp.float32)
            for t in range(acts.shape[1]):
                total = total + jnp.dot(
                    acts[k, t, n],
                    down_w[n, t * units : (t + 1) * units, :],
                    preferred_element_type=jnp.float32,
                )
            weighted[n] = total.reshape(2, capacity, down_w.shape[2])

        def combined(j):
            ones, scale = chosen(2 * s + j)
            value = jnp.concatenate([weighted[n, j] for n in range(local_count)], axis=0)
            value = (value * scale).astype(jnp.bfloat16)
            return lax.dot_general(
                ones, value, (((0,), (0,)), ((), ())), preferred_element_type=jnp.float32
            )

        pair_out[k] = combined(1 - core).astype(jnp.bfloat16)
        sums[k] = go(
            remote(pair_out.at[k], pair_in.at[k], sum_send.at[k], sum_recv.at[k], place(mate, tp))
        )
        mine = combined(core)
        sums[k].wait_recv()
        both = mine + pair_in[k].astype(jnp.float32)
        if k == 0:
            total_ref[...] = both
        else:
            back_out[k] = both.astype(jnp.bfloat16)
            backs[k] = go(
                remote(
                    back_out.at[k],
                    back_in.at[k],
                    back_send.at[k],
                    back_recv.at[k],
                    place(s * 2 + core, tp),
                )
            )

    backs = {}

    own_meta.wait()
    for copy in metas:
        copy.wait_recv()
    own_tok.wait()
    own_pair.wait_recv()
    loads[0].wait()
    loads[1].wait()
    first_half(0)
    send_act(0)
    loads[2].wait()
    for k in range(1, chips):
        spread_line(k)
        forward_act(k - 1)
        spread_side(k)
        first_half(k)
        send_act(k)
        if k >= 2:
            second_half(k - 2)
    forward_act(chips - 1)
    for k in range(max(chips - 2, 0), chips):
        second_half(k)
    result = total_ref[...]
    for k in range(1, chips):
        backs[k].wait_recv()
        result = result + back_in[k].astype(jnp.float32)
    out_ref[...] = result.astype(out_ref.dtype)
    for copy in pending:
        copy.wait_send()


def fused_per_device(tokens, norm_gain, route_ids, route_weights, w_gate, w_up, w_down):
    local_count, width, units = w_gate.shape
    out_cols = w_down.shape[2]
    sources = lax.axis_size("ep")
    tp_count = lax.axis_size("tp")
    experts = local_count * sources
    tok_rows, top_count = route_ids.shape
    capacity = 3 * tok_rows * top_count // (2 * experts)
    chips = sources // 2
    half = width // 2
    values = tokens.astype(jnp.float32)
    row_mean = jnp.mean(values, axis=1, keepdims=True)
    centred = values - row_mean
    row_var = jnp.mean(centred * centred, axis=1, keepdims=True)
    normed = (centred * lax.rsqrt(row_var + norm_eps) * norm_gain).astype(jnp.bfloat16)
    normed = jnp.stack([normed[:, :half], normed[:, half:]], axis=0)
    hits = route_ids[:, :, None] == jnp.arange(experts, dtype=jnp.int32)[None, None, :]
    named = jnp.any(hits, axis=1)
    weight_of = jnp.sum(jnp.where(hits, route_weights[:, :, None], 0.0), axis=1)
    order = jnp.arange(tok_rows)
    before = (order[:, None] > order[None, :]).astype(jnp.bfloat16)
    slot = jnp.dot(before, named.astype(jnp.bfloat16), preferred_element_type=jnp.float32)
    slot = jnp.where(named, slot, -1.0)
    pad = (-2 * local_count) % 8
    meta = jnp.concatenate(
        [
            slot.T.reshape(sources, local_count, tok_rows),
            weight_of.T.reshape(sources, local_count, tok_rows),
            jnp.zeros((sources, pad, tok_rows), jnp.float32),
        ],
        axis=1,
    )
    dma = pltpu.SemaphoreType.DMA
    bf16 = jnp.bfloat16
    vmem = pl.BlockSpec(memory_space=pltpu.VMEM)
    hbm = pl.BlockSpec(memory_space=pltpu.HBM)
    return pl.pallas_call(
        functools.partial(layer_kernel, capacity),
        out_shape=jax.ShapeDtypeStruct((tok_rows, out_cols), bf16),
        in_specs=[vmem, vmem, hbm, hbm, hbm],
        out_specs=vmem,
        scratch_shapes=[
            pltpu.VMEM(w_gate.shape, bf16),
            pltpu.VMEM(w_up.shape, bf16),
            pltpu.VMEM(w_down.shape, bf16),
            pltpu.VMEM((sources, 2, tok_rows, half), bf16),
            pltpu.VMEM(meta.shape, jnp.float32),
            pltpu.VMEM((local_count, 2, capacity, width), bf16),
            pltpu.VMEM((chips, tp_count, local_count, 2 * capacity, units), bf16),
            pltpu.VMEM((local_count, 2, capacity, out_cols), jnp.float32),
            pltpu.VMEM((chips, tok_rows, out_cols), bf16),
            pltpu.VMEM((chips, tok_rows, out_cols), bf16),
            pltpu.VMEM((chips, tok_rows, out_cols), bf16),
            pltpu.VMEM((chips, tok_rows, out_cols), bf16),
            pltpu.VMEM((tok_rows, out_cols), jnp.float32),
            dma((3,)),
            dma((2,)),
            dma((sources,)),
            dma((sources,)),
            dma((chips,)),
            dma((chips,)),
            dma((chips,)),
            dma((chips,)),
            dma((2 * chips,)),
            dma((2 * chips,)),
            dma((chips, 3)),
            dma((chips, 3)),
            dma((chips,)),
            dma((chips,)),
            dma((chips,)),
            dma((chips,)),
        ],
        compiler_params=pltpu.CompilerParams(
            collective_id=0, has_side_effects=True, vmem_limit_bytes=60 * 1024 * 1024
        ),
    )(normed, meta, w_gate, w_up, w_down)


def pick_plan(mesh):
    sources, tp_count = mesh.shape["ep"], mesh.shape["tp"]

    def body(tokens, norm_gain, route_ids, route_weights, w_gate, w_up, w_down):
        tok_rows, top_count = route_ids.shape
        experts = w_gate.shape[0] * sources
        capacity = 3 * tok_rows * top_count // (2 * experts)
        gathered = 2 * tokens.size * sources + 6 * w_gate.size
        fused = (
            tp_count == 4
            and sources in (4, 8)
            and capacity % 16 == 0
            and gathered < 32 * 1024 * 1024
        )
        run = fused_per_device if fused else per_device
        return run(tokens, norm_gain, route_ids, route_weights, w_gate, w_up, w_down)

    return body


def solution(mesh):
    return jax.shard_map(
        pick_plan(mesh),
        mesh=mesh,
        in_specs=(
            P("ep", None),
            P(),
            P("ep", None),
            P("ep", None),
            P("ep", None, "tp"),
            P("ep", None, "tp"),
            P("ep", None, "tp"),
        ),
        out_specs=P("ep", "tp"),
        check_vma=False,
    )
```

```python
import functools
import jax
import jax.numpy as jnp
from jax import lax
from jax.experimental import pallas as pl
from jax.experimental.pallas import tpu as pltpu
from jax.sharding import PartitionSpec as P

swiglu_limit = 7.0
swiglu_alpha = 1.702
norm_eps = 1e-05


def clamped_units(gate_pre, up_pre):
    capped = jnp.minimum(gate_pre, swiglu_limit)
    linear = jnp.clip(up_pre, -swiglu_limit, swiglu_limit)
    return capped * jax.nn.sigmoid(swiglu_alpha * capped) * (linear + 1.0)


def expert_work(outgoing, gate_weight, up_weight, down_weight):
    received = lax.all_to_all(outgoing, "ep", split_axis=1, concat_axis=1, tiled=True)
    local_count, sources, capacity, columns = received.shape
    row_count = sources * capacity
    row_block = received.reshape(local_count, row_count, columns)
    shard_piece = lax.all_gather(row_block, "tp", axis=2, tiled=True)
    gate_sum = jnp.einsum(
        "lrd,ldf->lrf", shard_piece, gate_weight, preferred_element_type=jnp.float32
    )
    up_sum = jnp.einsum("lrd,ldf->lrf", shard_piece, up_weight, preferred_element_type=jnp.float32)
    activation = clamped_units(gate_sum, up_sum).astype(jnp.bfloat16)
    out_cols = down_weight.shape[2]
    result = jnp.einsum(
        "lrf,lfd->lrd",
        lax.all_gather(activation, "tp", axis=2, tiled=True),
        down_weight,
        preferred_element_type=jnp.float32,
    )
    result = result.astype(jnp.bfloat16).reshape(local_count, sources, capacity, out_cols)
    return lax.all_to_all(result, "ep", split_axis=1, concat_axis=1, tiled=True)


def per_device(tokens, norm_gain, route_ids, route_weights, w_gate, w_up, w_down):
    local_count = w_gate.shape[0]
    sources = lax.axis_size("ep")
    tp_count = lax.axis_size("tp")
    width = tokens.shape[1]
    columns = width // tp_count
    experts = local_count * sources
    tok_rows, top_count = route_ids.shape
    capacity = 3 * tok_rows * top_count // (2 * experts)
    values = tokens.astype(jnp.float32)
    row_mean = jnp.mean(values, axis=1, keepdims=True)
    centred = values - row_mean
    row_var = jnp.mean(centred * centred, axis=1, keepdims=True)
    offset = lax.axis_index("tp") * columns
    own_cols = lax.dynamic_slice_in_dim(centred, offset, columns, 1)
    own_gain = lax.dynamic_slice_in_dim(norm_gain, offset, columns, 0)
    normed = (own_cols * lax.rsqrt(row_var + norm_eps) * own_gain).astype(jnp.bfloat16)
    flat_ids = route_ids.reshape(-1)
    matches = (flat_ids[:, None] == jnp.arange(experts, dtype=jnp.int32)[None, :]).astype(jnp.int32)
    earlier = jnp.cumsum(matches, axis=0) - matches
    slot_index = jnp.sum(earlier * matches, axis=1)
    position = (
        flat_ids % local_count * (sources * capacity)
        + flat_ids // local_count * capacity
        + slot_index
    )
    buffer_rows = local_count * sources * capacity
    placed = (
        position.reshape(tok_rows, top_count)[:, :, None]
        == jnp.arange(buffer_rows, dtype=jnp.int32)[None, None, :]
    )
    placement_matrix = jnp.any(placed, axis=1).astype(jnp.bfloat16)
    outgoing = jnp.einsum("tp,td->pd", placement_matrix, normed, preferred_element_type=jnp.float32)
    outgoing = outgoing.astype(jnp.bfloat16).reshape(local_count, sources, capacity, columns)
    returned = jnp.concatenate(
        [
            expert_work(
                outgoing[number : number + 1],
                w_gate[number : number + 1],
                w_up[number : number + 1],
                w_down[number : number + 1],
            )
            for number in range(local_count)
        ],
        axis=0,
    )
    flat_out = returned.reshape(buffer_rows, columns)
    picked = flat_out[position].reshape(tok_rows, top_count, columns).astype(jnp.float32)
    return jnp.sum(picked * route_weights[:, :, None], axis=1).astype(jnp.bfloat16)


def layer_kernel(
    capacity,
    normed_ref,
    meta_ref,
    gate_hbm,
    up_hbm,
    down_hbm,
    out_ref,
    gate_w,
    up_w,
    down_w,
    toks,
    meta_in,
    rows,
    acts,
    weighted,
    pair_out,
    pair_in,
    back_out,
    back_in,
    total_ref,
    weight_sem,
    local_sem,
    meta_send,
    meta_recv,
    line_send,
    line_recv,
    side_send,
    side_recv,
    pair_send,
    pair_recv,
    act_send,
    act_recv,
    sum_send,
    sum_recv,
    back_send,
    back_recv,
):
    sources = meta_ref.shape[0]
    chips = sources // 2
    local_count = gate_w.shape[0]
    units = gate_w.shape[2]
    tok_rows = normed_ref.shape[1]
    me = lax.axis_index("ep")
    tp = lax.axis_index("tp")
    z, core = me // 2, me % 2
    y, x = tp // 2, tp % 2
    tp_x = y * 2 + (1 - x)
    tp_y = (1 - y) * 2 + x
    tp_xy = (1 - y) * 2 + (1 - x)
    mate = z * 2 + (1 - core)
    own_half = (x + y) % 2

    def partner(k):
        chosen_chip = 0 * z
        for at in range(chips):
            order = sorted(range(chips), key=lambda c: (abs(c - at), c))
            gap = (z - at) * (z - at)
            chosen_chip = chosen_chip + order[k] * (1 - (gap + chips * chips - 1) // (chips * chips))
        return chosen_chip

    def place(ep, column):
        return {"ep": ep, "tp": column}

    def remote(source, target, send, recv, where):
        return pltpu.make_async_remote_copy(
            src_ref=source,
            dst_ref=target,
            send_sem=send,
            recv_sem=recv,
            device_id=where,
            device_id_type=pl.DeviceIdType.MESH,
        )

    loads = []
    for n, (hbm, vmem) in enumerate(((gate_hbm, gate_w), (up_hbm, up_w), (down_hbm, down_w))):
        loads.append(pltpu.make_async_copy(hbm, vmem, weight_sem.at[n]))
        loads[-1].start()
    own_tok = pltpu.make_async_copy(normed_ref, toks.at[me], local_sem.at[0])
    own_tok.start()
    own_meta = pltpu.make_async_copy(meta_ref.at[me], meta_in.at[me], local_sem.at[1])
    own_meta.start()

    barrier = pltpu.get_barrier_semaphore()
    for d in range(1, sources):
        pl.semaphore_signal(
            barrier, inc=1, device_id=place((me + d) % sources, tp), device_id_type=pl.DeviceIdType.MESH
        )
    for column in (tp_x, tp_y):
        pl.semaphore_signal(
            barrier, inc=1, device_id=place(me, column), device_id_type=pl.DeviceIdType.MESH
        )
    pl.semaphore_wait(barrier, sources + 1)

    pending = []

    def go(copy):
        copy.start()
        pending.append(copy)
        return copy

    metas = [
        go(
            remote(
                meta_ref.at[(me + d) % sources],
                meta_in.at[me],
                meta_send.at[d],
                meta_recv.at[d],
                place((me + d) % sources, tp),
            )
        )
        for d in range(1, sources)
    ]
    own_pair = go(
        remote(normed_ref, toks.at[me], pair_send.at[0], pair_recv.at[0], place(mate, tp))
    )
    def line(chip, up, distance):
        piece = toks.at[chip * 2 + core, own_half]
        return remote(
            normed_ref.at[own_half] if distance is None else piece,
            piece,
            line_send.at[up, chip],
            line_recv.at[up, chip],
            place((z + 2 * up - 1) * 2 + core, tp),
        )

    @pl.when(z < chips - 1)
    def _():
        line(z, 1, None).start()

    @pl.when(z > 0)
    def _():
        line(z, 0, None).start()

    def upward(chip):
        return (chips + z - chip - 1) // chips

    def goes_on(chip):
        ahead = z + 2 * upward(chip) - 1
        return jnp.logical_and(ahead >= 0, ahead < chips)

    pairs, sides, half_pairs = {}, {}, {}
    cut_rows = tok_rows // 2

    def spread_line(k):
        chip = partner(k)
        src = chip * 2 + core
        up = upward(chip)
        line(chip, up, k).wait_recv()

        @pl.when(goes_on(chip))
        def _():
            line(chip, up, k).start()

        sides[k] = []
        for n, column in enumerate((tp_x, tp_y)):
            part = toks.at[src, own_half, pl.ds(n * cut_rows, cut_rows)]
            sides[k].append(
                go(remote(part, part, side_send.at[k, n], side_recv.at[k, n], place(me, column)))
            )
        piece = toks.at[src, own_half]
        pairs[k] = go(
            remote(piece, piece, pair_send.at[2 * k], pair_recv.at[2 * k], place(mate, tp))
        )

    def spread_side(k):
        src = partner(k) * 2 + core
        for copy in sides[k]:
            copy.wait_recv()
        piece = toks.at[src, 1 - own_half]
        half_pairs[k] = go(
            remote(piece, piece, pair_send.at[2 * k + 1], pair_recv.at[2 * k + 1], place(mate, tp))
        )

    def settle(k):
        pairs[k].wait_recv()
        half_pairs[k].wait_recv()

    def chosen(source):
        slots = meta_in[source]
        at = lax.broadcasted_iota(jnp.int32, (capacity, tok_rows), 0).astype(jnp.float32)
        hits = [at == slots[n : n + 1, :] for n in range(local_count)]
        ones = jnp.concatenate([h.astype(jnp.float32) for h in hits], axis=0)
        scale = jnp.concatenate(
            [
                jnp.sum(
                    jnp.where(hits[n], slots[local_count + n : local_count + n + 1, :], 0.0),
                    axis=1,
                    keepdims=True,
                )
                for n in range(local_count)
            ],
            axis=0,
        )
        return ones.astype(jnp.bfloat16), scale

    halves = toks.shape[1]
    width = toks.shape[3]

    def first_half(k):
        s = partner(k)

        @pl.loop(0, 2)
        def _(j):
            ones, _ = chosen(2 * s + j)
            for h in range(halves):
                got = jnp.dot(ones, toks[2 * s + j, h], preferred_element_type=jnp.float32)
                got = got.astype(jnp.bfloat16)
                for n in range(local_count):
                    rows[n, j, :, h * width : (h + 1) * width] = got[
                        n * capacity : (n + 1) * capacity
                    ]

        @pl.loop(0, local_count)
        def _(n):
            block = rows[n].reshape(2 * capacity, halves * width)
            cut = units // 2
            for part in range(2):
                cols = slice(part * cut, (part + 1) * cut)
                gate = jnp.dot(block, gate_w[n, :, cols], preferred_element_type=jnp.float32)
                up = jnp.dot(block, up_w[n, :, cols], preferred_element_type=jnp.float32)
                acts[k, tp, n, :, cols] = clamped_units(gate, up).astype(jnp.bfloat16)

    own_x, own_y, fwd_y, fwd_x = {}, {}, {}, {}

    def send_act(k):
        piece = acts.at[k, tp]
        own_x[k] = go(
            remote(piece, piece, act_send.at[k, 0], act_recv.at[k, 0], place(me, tp_x))
        )
        own_y[k] = go(
            remote(piece, piece, act_send.at[k, 1], act_recv.at[k, 1], place(me, tp_y))
        )

    def forward_act(k):
        mid = local_count // 2
        own_x[k].wait_recv()
        piece = acts.at[k, tp_x, pl.ds(0, mid)]
        fwd_y[k] = go(
            remote(piece, piece, act_send.at[k, 2], act_recv.at[k, 2], place(me, tp_y))
        )
        own_y[k].wait_recv()
        piece = acts.at[k, tp_y, pl.ds(mid, local_count - mid)]
        fwd_x[k] = go(
            remote(piece, piece, act_send.at[k, 3], act_recv.at[k, 3], place(me, tp_x))
        )

    sums = {}

    def second_half(k):
        s = partner(k)
        fwd_y[k].wait_recv()
        fwd_x[k].wait_recv()

        @pl.loop(0, local_count)
        def _(n):
            total = jnp.zeros((2 * capacity, down_w.shape[2]), jnp.float32)
            for t in range(acts.shape[1]):
                total = total + jnp.dot(
                    acts[k, t, n],
                    down_w[n, t * units : (t + 1) * units, :],
                    preferred_element_type=jnp.float32,
                )
            weighted[n] = total.reshape(2, capacity, down_w.shape[2])

        def combined(j):
            ones, scale = chosen(2 * s + j)
            value = jnp.concatenate([weighted[n, j] for n in range(local_count)], axis=0)
            value = (value * scale).astype(jnp.bfloat16)
            return lax.dot_general(
                ones, value, (((0,), (0,)), ((), ())), preferred_element_type=jnp.float32
            )

        pair_out[k] = combined(1 - core).astype(jnp.bfloat16)
        sums[k] = go(
            remote(pair_out.at[k], pair_in.at[k], sum_send.at[k], sum_recv.at[k], place(mate, tp))
        )
        mine = combined(core)
        sums[k].wait_recv()
        both = mine + pair_in[k].astype(jnp.float32)
        if k == 0:
            total_ref[...] = both
        else:
            back_out[k] = both.astype(jnp.bfloat16)
            go(
                remote(
                    back_out.at[k],
                    back_in.at[z],
                    back_send.at[k],
                    back_recv.at[z],
                    place(s * 2 + core, tp),
                )
            )


    own_meta.wait()
    for copy in metas:
        copy.wait_recv()
    own_tok.wait()
    own_pair.wait_recv()
    loads[0].wait()
    loads[1].wait()
    first_half(0)
    send_act(0)
    loads[2].wait()
    spread_line(1)
    forward_act(0)
    if chips > 2:
        spread_line(2)
    for k in range(1, chips):
        spread_side(k)
        if k + 2 < chips:
            spread_line(k + 2)
        settle(k)
        first_half(k)
        send_act(k)
        second_half(k - 1)
        forward_act(k)
    second_half(chips - 1)
    result = total_ref[...]
    for k in range(1, chips):
        other = (z + k) % chips
        remote(
            back_out.at[k], back_in.at[other], back_send.at[k], back_recv.at[other], place(mate, tp)
        ).wait_recv()
        result = result + back_in[other].astype(jnp.float32)
    out_ref[...] = result.astype(out_ref.dtype)
    for copy in pending:
        copy.wait_send()

    @pl.when(z < chips - 1)
    def _():
        line(z, 1, None).wait_send()

    @pl.when(z > 0)
    def _():
        line(z, 0, None).wait_send()

    for k in range(1, chips):
        chip = partner(k)

        @pl.when(goes_on(chip))
        def _():
            line(chip, upward(chip), k).wait_send()


def fused_per_device(tokens, norm_gain, route_ids, route_weights, w_gate, w_up, w_down):
    local_count, width, units = w_gate.shape
    out_cols = w_down.shape[2]
    sources = lax.axis_size("ep")
    tp_count = lax.axis_size("tp")
    experts = local_count * sources
    tok_rows, top_count = route_ids.shape
    capacity = 3 * tok_rows * top_count // (2 * experts)
    chips = sources // 2
    half = width // 2
    values = tokens.astype(jnp.float32)
    row_mean = jnp.mean(values, axis=1, keepdims=True)
    centred = values - row_mean
    row_var = jnp.mean(centred * centred, axis=1, keepdims=True)
    normed = (centred * lax.rsqrt(row_var + norm_eps) * norm_gain).astype(jnp.bfloat16)
    normed = jnp.stack([normed[:, :half], normed[:, half:]], axis=0)
    hits = route_ids[:, :, None] == jnp.arange(experts, dtype=jnp.int32)[None, None, :]
    named = jnp.any(hits, axis=1)
    weight_of = jnp.sum(jnp.where(hits, route_weights[:, :, None], 0.0), axis=1)
    order = jnp.arange(tok_rows)
    before = (order[:, None] > order[None, :]).astype(jnp.bfloat16)
    slot = jnp.dot(before, named.astype(jnp.bfloat16), preferred_element_type=jnp.float32)
    slot = jnp.where(named, slot, -1.0)
    pad = (-2 * local_count) % 8
    meta = jnp.concatenate(
        [
            slot.T.reshape(sources, local_count, tok_rows),
            weight_of.T.reshape(sources, local_count, tok_rows),
            jnp.zeros((sources, pad, tok_rows), jnp.float32),
        ],
        axis=1,
    )
    dma = pltpu.SemaphoreType.DMA
    bf16 = jnp.bfloat16
    vmem = pl.BlockSpec(memory_space=pltpu.VMEM)
    hbm = pl.BlockSpec(memory_space=pltpu.HBM)
    return pl.pallas_call(
        functools.partial(layer_kernel, capacity),
        out_shape=jax.ShapeDtypeStruct((tok_rows, out_cols), bf16),
        in_specs=[vmem, vmem, hbm, hbm, hbm],
        out_specs=vmem,
        scratch_shapes=[
            pltpu.VMEM(w_gate.shape, bf16),
            pltpu.VMEM(w_up.shape, bf16),
            pltpu.VMEM(w_down.shape, bf16),
            pltpu.VMEM((sources, 2, tok_rows, half), bf16),
            pltpu.VMEM(meta.shape, jnp.float32),
            pltpu.VMEM((local_count, 2, capacity, width), bf16),
            pltpu.VMEM((chips, tp_count, local_count, 2 * capacity, units), bf16),
            pltpu.VMEM((local_count, 2, capacity, out_cols), jnp.float32),
            pltpu.VMEM((chips, tok_rows, out_cols), bf16),
            pltpu.VMEM((chips, tok_rows, out_cols), bf16),
            pltpu.VMEM((chips, tok_rows, out_cols), bf16),
            pltpu.VMEM((chips, tok_rows, out_cols), bf16),
            pltpu.VMEM((tok_rows, out_cols), jnp.float32),
            dma((3,)),
            dma((2,)),
            dma((sources,)),
            dma((sources,)),
            dma((2, chips)),
            dma((2, chips)),
            dma((chips, 2)),
            dma((chips, 2)),
            dma((2 * chips,)),
            dma((2 * chips,)),
            dma((chips, 4)),
            dma((chips, 4)),
            dma((chips,)),
            dma((chips,)),
            dma((chips,)),
            dma((chips,)),
        ],
        compiler_params=pltpu.CompilerParams(
            collective_id=0, has_side_effects=True, vmem_limit_bytes=60 * 1024 * 1024
        ),
    )(normed, meta, w_gate, w_up, w_down)


def pick_plan(mesh):
    sources, tp_count = mesh.shape["ep"], mesh.shape["tp"]

    def body(tokens, norm_gain, route_ids, route_weights, w_gate, w_up, w_down):
        tok_rows, top_count = route_ids.shape
        experts = w_gate.shape[0] * sources
        capacity = 3 * tok_rows * top_count // (2 * experts)
        gathered = 2 * tokens.size * sources + 6 * w_gate.size
        fused = (
            tp_count == 4
            and sources in (4, 8)
            and capacity % 16 == 0
            and w_gate.shape[0] % 2 == 0
            and tok_rows % 32 == 0
            and gathered < 32 * 1024 * 1024
        )
        run = fused_per_device if fused else per_device
        return run(tokens, norm_gain, route_ids, route_weights, w_gate, w_up, w_down)

    return body


def solution(mesh):
    return jax.shard_map(
        pick_plan(mesh),
        mesh=mesh,
        in_specs=(
            P("ep", None),
            P(),
            P("ep", None),
            P("ep", None),
            P("ep", None, "tp"),
            P("ep", None, "tp"),
            P("ep", None, "tp"),
        ),
        out_specs=P("ep", "tp"),
        check_vma=False,
    )
```
